512 devices in a mesh: rep: 2 (over z_hi), fs: 32 (over z_lo, y), tp: 8 (over x, core).
Axes of the slice: x: 4, y: 8, z: 8 (z_hi: 2, z_lo: 4; z = z_hi * 4 + z_lo), core: 2. Of those that a mesh axis runs over, the one named last changes fastest.
Arguments:
- tokens: bfloat16 [24576, 2048], P(('rep', 'fs'), 'tp'), may hold values from -6 to 6
- mixing_norm_gain: float32 [2048], replicated, may hold values from 0.1 to 1.9
- recurrent_input_weight: float32 [2048, 3072], P('fs', 'tp'), may hold values from -0.125 to 0.125
- recurrent_input_scale: float32 [3072], P('tp'), may hold values from 0.5 to 2
- convolution_kernel_taps: float32 [4, 3072], P(None, 'tp'), may hold values from -3 to 3
- recurrence_gate_weight_blocks: bfloat16 [24, 128, 128], P('tp'), may hold values from -0.5 to 0.5
- input_gate_weight_blocks: bfloat16 [24, 128, 128], P('tp'), may hold values from -0.5 to 0.5
- channel_decay_parameter: float32 [3072], P('tp'), may hold values from 3 to 9
- token_extra_log_decay: float32 [24576], P(('rep', 'fs')), may hold values from -0.7 to 0
- mixing_output_weight: float32 [3072, 2048], P('tp', 'fs'), may hold values from -0.109375 to 0.109375
- mixing_output_scale: float32 [2048], P('fs'), may hold values from 0.5 to 2
- feedforward_norm_gain: float32 [2048], replicated, may hold values from 0.1 to 1.9
- feedforward_gate_weight: float32 [2048, 5120], P('fs', 'tp'), may hold values from -0.125 to 0.125
- feedforward_gate_scale: float32 [5120], P('tp'), may hold values from 0.5 to 2
- feedforward_up_weight: float32 [2048, 5120], P('fs', 'tp'), may hold values from -0.125 to 0.125
- feedforward_up_scale: float32 [5120], P('tp'), may hold values from 0.5 to 2
- feedforward_down_weight: float32 [5120, 2048], P('tp', 'fs'), may hold values from -0.078125 to 0.078125
- feedforward_down_scale: float32 [2048], P('fs'), may hold values from 0.5 to 2
Outputs:
- layer_out: bfloat16 [24576, 2048], P(('rep', 'fs'), 'tp')
The draws below stay inside these ranges and needn't reach their ends.
All inputs are finite; a program needn't handle non-finite values.
Results may differ from the reference program's by a relative error of at most 0.02.
Values may be sent and summed in bfloat16 or wider, within the bound.
No kernel may reach another device: no remote copies, remote signals or barrier semaphores. Data moves between devices by JAX's collectives and lax.ppermute only.
A program may use at most 64 MiB of HBM per device.

```python
import math
import jax
import jax.numpy as jnp
from jax import lax

MODEL_DIM = 2048
W = 3072
FF = 5120
BLOCK = 128
CONV = 4
SEQUENCE_LENGTH = 384
NB = 24
TOKENS = 24576
N_TP = 8


def draw_token_extra_log_decay(key, part):
    first_key, second_key = jax.random.split(jax.random.fold_in(key, 17))
    chosen = jax.random.randint(first_key, (TOKENS,), 0, 64) == 0
    depth = jax.random.uniform(second_key, (TOKENS,), jnp.float32, 0.22, 0.7)
    return jnp.where(chosen, -depth, 0.0).astype(jnp.float32)


def block_levels(key, dims, pieces, least, high):
    level = 1.0
    for dim, shards_of in pieces:
        draws = jax.random.uniform(jax.random.fold_in(jax.random.fold_in(key, 6), dim), (shards_of,), jnp.float32, least / len(pieces), high / len(pieces))
        level = level * jnp.repeat(jnp.exp(draws), dims[dim] // shards_of).reshape((-1,) + (1,) * (len(dims) - 1 - dim))
    return level


def scatter_about(key, extent, scale, reach, pieces=(), held_as=jnp.bfloat16):
    result = jax.random.normal(key, extent, jnp.float32) * scale
    if len(pieces) > 0:
        result = block_levels(key, extent, pieces, -0.22, 0.18) * result
    return jnp.clip(result, min=-reach, max=reach).astype(held_as)


def setup_inputs(seed: int = 0) -> dict:
    key_of = jax.random.split(jax.random.key(seed), 19)
    return {
        "tokens": scatter_about(key_of[0], (TOKENS, MODEL_DIM), 1.0, 6.0, ((0, 64), (1, 8))),
        "mixing_norm_gain": jnp.clip(1.0 + 0.18 * jax.random.normal(key_of[1], (MODEL_DIM,), jnp.float32), 0.1, 1.9),
        "recurrent_input_weight": scatter_about(key_of[2], (MODEL_DIM, W), MODEL_DIM ** -0.5, 0.125, ((0, 32), (1, 8)), jnp.float32),
        "recurrent_input_scale": jnp.clip(jnp.exp(math.log(2.0) - 1.3862944 * jax.random.uniform(key_of[3], (W,), jnp.float32) ** block_levels(key_of[3], (W,), ((0, 8),), -0.2, 0.2)), 0.5, 2.0),
        "convolution_kernel_taps": scatter_about(key_of[4], (CONV, W), 0.5, 3.0, ((1, 8),), jnp.float32),
        "recurrence_gate_weight_blocks": scatter_about(key_of[5], (NB, BLOCK, BLOCK), BLOCK ** -0.5, 0.5, ((0, 8),)),
        "input_gate_weight_blocks": scatter_about(key_of[6], (NB, BLOCK, BLOCK), BLOCK ** -0.5, 0.5, ((0, 8),)),
        "channel_decay_parameter": jnp.clip(3.0 + 6.0 * jax.random.uniform(key_of[7], (W,), jnp.float32) ** block_levels(key_of[7], (W,), ((0, 8),), -0.2, 0.2), 3.0, 9.0),
        "token_extra_log_decay": draw_token_extra_log_decay(jax.random.fold_in(key_of[18], 71), 0),
        "mixing_output_weight": scatter_about(key_of[9], (W, MODEL_DIM), W ** -0.5, 0.109375, ((0, 8), (1, 32)), jnp.float32),
        "mixing_output_scale": jnp.clip(jnp.exp(math.log(2.0) - 1.3862944 * jax.random.uniform(key_of[10], (MODEL_DIM,), jnp.float32) ** block_levels(key_of[10], (MODEL_DIM,), ((0, 32),), -0.2, 0.2)), 0.5, 2.0),
        "feedforward_norm_gain": jnp.clip(1.0 + 0.18 * jax.random.normal(key_of[11], (MODEL_DIM,), jnp.float32), 0.1, 1.9),
        "feedforward_gate_weight": scatter_about(key_of[12], (MODEL_DIM, FF), MODEL_DIM ** -0.5, 0.125, ((0, 32), (1, 8)), jnp.float32),
        "feedforward_gate_scale": jnp.clip(jnp.exp(math.log(2.0) - 1.3862944 * jax.random.uniform(key_of[13], (FF,), jnp.float32) ** block_levels(key_of[13], (FF,), ((0, 8),), -0.2, 0.2)), 0.5, 2.0),
        "feedforward_up_weight": scatter_about(key_of[14], (MODEL_DIM, FF), MODEL_DIM ** -0.5, 0.125, ((0, 32), (1, 8)), jnp.float32),
        "feedforward_up_scale": jnp.clip(jnp.exp(math.log(2.0) - 1.3862944 * jax.random.uniform(key_of[15], (FF,), jnp.float32) ** block_levels(key_of[15], (FF,), ((0, 8),), -0.2, 0.2)), 0.5, 2.0),
        "feedforward_down_weight": scatter_about(key_of[16], (FF, MODEL_DIM), FF ** -0.5, 0.078125, ((0, 8), (1, 32)), jnp.float32),
        "feedforward_down_scale": jnp.clip(jnp.exp(math.log(2.0) - 1.3862944 * jax.random.uniform(key_of[17], (MODEL_DIM,), jnp.float32) ** block_levels(key_of[17], (MODEL_DIM,), ((0, 32),), -0.2, 0.2)), 0.5, 2.0),
    }


EPS = 1e-06
DECAY_FACTOR = 8.0

def row_norm(rows, gain_vec):
    values = rows.astype(jnp.float32)
    inverse = lax.rsqrt(lax.optimization_barrier(jnp.mean(values * values, axis=-1, keepdims=True)) + EPS)
    return (values * inverse * gain_vec).astype(jnp.bfloat16)

def combine_pairs(earlier, later):
    decay_one, value_one = earlier
    decay_two, value_two = later
    return (decay_one * decay_two, decay_two * value_one + value_two)

def grouped_sum(left_rows, weight_low, col_scale, groups):
    seq_rows, inner = left_rows.shape
    left_groups = left_rows.reshape(seq_rows, groups, inner // groups).astype(jnp.float32)
    weight_groups = weight_low.reshape(groups, inner // groups, weight_low.shape[1]).astype(jnp.float32)
    parts = jnp.einsum('lgw,gwd->gld', left_groups, weight_groups) * col_scale
    parts_low = parts.astype(jnp.bfloat16)
    parts_low = lax.optimization_barrier(parts_low)
    return lax.optimization_barrier(jnp.sum(parts_low.astype(jnp.float32), axis=0))

def reference(tokens, mixing_norm_gain, recurrent_input_weight, recurrent_input_scale, convolution_kernel_taps, recurrence_gate_weight_blocks, input_gate_weight_blocks, channel_decay_parameter, token_extra_log_decay, mixing_output_weight, mixing_output_scale, feedforward_norm_gain, feedforward_gate_weight, feedforward_gate_scale, feedforward_up_weight, feedforward_up_scale, feedforward_down_weight, feedforward_down_scale):
    rec_low = recurrent_input_weight.astype(jnp.bfloat16)
    mix_low = mixing_output_weight.astype(jnp.bfloat16)
    gate_low = feedforward_gate_weight.astype(jnp.bfloat16)
    up_low = feedforward_up_weight.astype(jnp.bfloat16)
    down_low = feedforward_down_weight.astype(jnp.bfloat16)
    recur_f32 = recurrence_gate_weight_blocks.astype(jnp.float32)
    input_f32 = input_gate_weight_blocks.astype(jnp.float32)

    def single_sequence(packed_arrays):
        sequence_token_rows, sequence_extra_decay = packed_arrays
        normed = row_norm(sequence_token_rows, mixing_norm_gain)
        rec_input = (jnp.dot(normed, rec_low, preferred_element_type=jnp.float32) * recurrent_input_scale).astype(jnp.bfloat16)
        rec_f32 = rec_input.astype(jnp.float32)
        padded = jnp.pad(rec_f32, ((CONV - 1, 0), (0, 0)))
        conv_out = jnp.zeros((SEQUENCE_LENGTH, W), jnp.float32)
        for tap_index in range(CONV):
            conv_out = conv_out + convolution_kernel_taps[tap_index] * padded[tap_index:tap_index + SEQUENCE_LENGTH]
        blocks = conv_out.astype(jnp.bfloat16).reshape(SEQUENCE_LENGTH, NB, BLOCK).astype(jnp.float32)
        recurrence_gate_values = jax.nn.sigmoid(jnp.einsum('lni,nij->lnj', blocks, recur_f32).reshape(SEQUENCE_LENGTH, W))
        input_gate = jax.nn.sigmoid(jnp.einsum('lni,nij->lnj', blocks, input_f32).reshape(SEQUENCE_LENGTH, W))
        decay_logarithm = -DECAY_FACTOR * recurrence_gate_values * jax.nn.softplus(-channel_decay_parameter) + sequence_extra_decay[:, None]
        decay = jnp.exp(decay_logarithm)
        drive = jnp.sqrt(-jnp.expm1(2.0 * decay_logarithm)) * input_gate * conv_out
        _, state = lax.associative_scan(combine_pairs, (decay, drive), axis=0)
        state_low = state.astype(jnp.bfloat16)
        mix_sum = grouped_sum(state_low, mix_low, mixing_output_scale, N_TP)
        mixed = (sequence_token_rows.astype(jnp.float32) + mix_sum).astype(jnp.bfloat16)
        normed_ffn = row_norm(mixed, feedforward_norm_gain)
        ffn_gate = jnp.dot(normed_ffn, gate_low, preferred_element_type=jnp.float32) * feedforward_gate_scale
        ffn_up = jnp.dot(normed_ffn, up_low, preferred_element_type=jnp.float32) * feedforward_up_scale
        hidden = (jax.nn.silu(ffn_gate) * ffn_up).astype(jnp.bfloat16)
        down_sum = grouped_sum(hidden, down_low, feedforward_down_scale, N_TP)
        return (mixed.astype(jnp.float32) + down_sum).astype(jnp.bfloat16)
    sequence_count = TOKENS // SEQUENCE_LENGTH
    output_list = lax.map(single_sequence, (tokens.reshape(sequence_count, SEQUENCE_LENGTH, MODEL_DIM), token_extra_log_decay.reshape(sequence_count, SEQUENCE_LENGTH)))
    return output_list.reshape(TOKENS, MODEL_DIM)
```

```python
import functools

import jax
import jax.numpy as jnp
from jax import lax
from jax.experimental import pallas as pl
from jax.experimental.pallas import tpu as pltpu
from jax.sharding import Mesh
from jax.sharding import PartitionSpec as P

FS = ("z", "y")
TP = ("x", "c")
REP_FS = ("rep", "z", "y")
EPS = 1e-06
DECAY_FACTOR = 8.0
CHUNKS = 8
F32 = jnp.float32
BF16 = jnp.bfloat16


def shift_z(value, step):
    count = lax.axis_size("rep") * lax.axis_size("z")
    return lax.ppermute(value, ("rep", "z"), [(i, (i + step) % count) for i in range(count)])


def copies_to(value, axis):
    copies = jnp.broadcast_to(value, (lax.axis_size(axis), *value.shape))
    return lax.all_to_all(copies, axis, split_axis=0, concat_axis=0, tiled=True)


def swap(value, axis):
    return lax.all_to_all(value, axis, split_axis=0, concat_axis=0, tiled=True)


def gather_features(block):
    return copies_to(copies_to(block, "x"), "c")


def share_sums(terms):
    pair = swap(terms, "c").astype(F32).sum(axis=0).astype(BF16)
    return swap(pair, "x").astype(F32).sum(axis=0)


def over_z(own):
    before = shift_z(own, 1)
    after = shift_z(own, -1)
    half = own.shape[0] // 2
    far_low = shift_z(after[:half], -1)
    far_high = shift_z(before[half:], 1)
    return own, before, after, far_low, far_high


def over_y(piece):
    return copies_to(piece, "y").reshape(-1, piece.shape[1])


def z_then_y(piece):
    near = (piece, shift_z(piece, 1), shift_z(piece, -1), shift_z(piece, 2))
    return lax.all_gather(jnp.concatenate(near, axis=1), "y", axis=0, tiled=True)


def dot(a, b):
    return jnp.dot(a, b, preferred_element_type=F32)


def dot_t(a, b):
    return lax.dot_general(a, b, (((1,), (1,)), ((), ())), preferred_element_type=F32)


def normalize(rows_ref, gain_ref, normed_ref):
    cores, chips, _, width = rows_ref.shape
    total = None
    for x in range(chips):
        for c in range(cores):
            v = rows_ref[c, x].astype(F32)
            part = jnp.sum(v * v, axis=-1, keepdims=True)
            total = part if total is None else total + part
    inverse = lax.rsqrt(total / (cores * chips * width) + EPS)
    for x in range(chips):
        for c in range(cores):
            cols = slice(c * width, (c + 1) * width)
            v = rows_ref[c, x].astype(F32)
            normed_ref[x, :, cols] = (v * inverse * gain_ref[x : x + 1, cols]).astype(BF16)


def recurrence_kernel(
    place_ref,
    rows_ref,
    gain_ref,
    own_ref,
    before_ref,
    after_ref,
    far_low_ref,
    far_high_ref,
    scale_ref,
    taps_ref,
    recur_ref,
    input_ref,
    rate_ref,
    extra_ref,
    out_ref,
    normed_ref,
    padded_ref,
    decay_ref,
    value_ref,
):
    rows = rows_ref.shape[2]
    width = scale_ref.shape[1]
    half = far_low_ref.shape[0]
    normalize(rows_ref, gain_ref, normed_ref)
    own, before, after, far = (place_ref[i] for i in range(4))
    total = dot(normed_ref[own], own_ref[:, :width])
    total += dot(normed_ref[before], before_ref[:, :width])
    total += dot(normed_ref[after], after_ref[:, :width])
    total += dot(normed_ref[far, :, :half], far_low_ref[:, :width])
    total += dot(normed_ref[far, :, half:], far_high_ref[:, :width])
    taps = taps_ref.shape[0]
    padded_ref[0:8, :] = jnp.zeros((8, width), F32)
    padded_ref[8:, :] = (total * scale_ref[...]).astype(BF16).astype(F32)
    conv = None
    for k in range(taps):
        start = 8 - (taps - 1) + k
        term = taps_ref[k : k + 1, :] * padded_ref[start : start + rows, :]
        conv = term if conv is None else conv + term
    low = conv.astype(BF16)
    size = recur_ref.shape[1]
    for n in range(recur_ref.shape[0]):
        cols = slice(n * size, (n + 1) * size)
        gate = jax.nn.sigmoid(dot(low[:, cols], recur_ref[n]))
        chosen = jax.nn.sigmoid(dot(low[:, cols], input_ref[n]))
        logarithm = gate * rate_ref[:, cols] + extra_ref[...]
        decay = jnp.exp(logarithm)
        rest = jnp.tanh(-logarithm) * (1.0 + decay * decay)
        decay_ref[n] = decay
        value_ref[n] = jnp.sqrt(rest) * chosen * conv[:, cols]
    count = recur_ref.shape[0]
    steps = rows // CHUNKS

    def step(t, carry):
        new = []
        for n in range(count):
            at = (n, pl.ds(t, CHUNKS, stride=steps), slice(None))
            decay = decay_ref[at]
            state = decay * carry[2 * n] + value_ref[at]
            product = decay * carry[2 * n + 1]
            value_ref[at] = state
            decay_ref[at] = product
            new += [state, product]
        return tuple(new)

    first = (jnp.zeros((CHUNKS, size), F32), jnp.ones((CHUNKS, size), F32)) * count
    ends = lax.fori_loop(0, steps, step, first, unroll=8)
    states = []
    for n in range(count):
        state, product = ends[2 * n], ends[2 * n + 1]
        enter = jnp.zeros((1, size), F32)
        pieces = []
        for chunk in range(CHUNKS):
            span = slice(chunk * steps, (chunk + 1) * steps)
            pieces.append((value_ref[n, span, :] + decay_ref[n, span, :] * enter).astype(BF16))
            enter = state[chunk : chunk + 1] + product[chunk : chunk + 1] * enter
        states.append(jnp.concatenate(pieces, axis=0))
    low = jnp.concatenate(states, axis=1)
    store(out_ref, own, dot_t(low, own_ref[:, width:]))
    store(out_ref, before, dot_t(low, before_ref[:, width:]))
    store(out_ref, after, dot_t(low, after_ref[:, width:]))
    out_ref[0, far] = dot_t(low, far_low_ref[:, width:]).astype(BF16)
    out_ref[1, far] = dot_t(low, far_high_ref[:, width:]).astype(BF16)


def store(out_ref, place, product):
    width = out_ref.shape[3]
    for c in range(out_ref.shape[0]):
        out_ref[c, place] = product[:, c * width : (c + 1) * width].astype(BF16)


def ffn_kernel(
    place_ref,
    rows_ref,
    gain_ref,
    weights_ref,
    gate_scale_ref,
    up_scale_ref,
    out_ref,
    normed_ref,
):
    normalize(rows_ref, gain_ref, normed_ref)
    width = gate_scale_ref.shape[1]
    block = 3 * width
    gate = up = None
    for k in range(4):
        left = normed_ref[place_ref[k]]
        g = dot(left, weights_ref[:, k * block : k * block + width])
        u = dot(left, weights_ref[:, k * block + width : k * block + 2 * width])
        gate, up = (g, u) if gate is None else (gate + g, up + u)
    gate = gate * gate_scale_ref[...]
    up = up * up_scale_ref[...]
    hidden = (gate * jax.nn.sigmoid(gate) * up).astype(BF16)
    for k in range(4):
        right = weights_ref[:, k * block + 2 * width : (k + 1) * block]
        store(out_ref, place_ref[k], dot_t(hidden, right))


def call(kernel, place, args, rows, width, scratch, flops):
    vmem = pl.BlockSpec(memory_space=pltpu.VMEM)
    return pl.pallas_call(
        kernel,
        out_shape=jax.ShapeDtypeStruct((2, 4, rows, width), BF16),
        in_specs=[pl.BlockSpec(memory_space=pltpu.SMEM)] + [vmem] * len(args),
        out_specs=vmem,
        scratch_shapes=[pltpu.VMEM((4, rows, 2 * width), BF16)] + scratch,
        compiler_params=pltpu.CompilerParams(vmem_limit_bytes=56 * 1024 * 1024),
        cost_estimate=pl.CostEstimate(flops=flops, transcendentals=0, bytes_accessed=0),
    )(place, *args)


def body(
    tokens,
    mixing_norm_gain,
    recurrent_input_weight,
    recurrent_input_scale,
    convolution_kernel_taps,
    recurrence_gate_weight_blocks,
    input_gate_weight_blocks,
    channel_decay_parameter,
    token_extra_log_decay,
    mixing_output_weight,
    mixing_output_scale,
    feedforward_norm_gain,
    feedforward_gate_weight,
    feedforward_gate_scale,
    feedforward_up_weight,
    feedforward_up_scale,
    feedforward_down_weight,
    feedforward_down_scale,
):
    rows, features = tokens.shape
    width = recurrent_input_weight.shape[1]
    z_count = lax.axis_size("z")
    z = lax.axis_index("z")
    place = jnp.stack([z, z + z_count - 1, z + 1, z + 2]).astype(jnp.int32) % z_count

    mix_rows = (mixing_output_weight * mixing_output_scale).T
    mixing = jnp.concatenate([recurrent_input_weight, mix_rows], axis=1).astype(BF16)
    down_rows = (feedforward_down_weight * feedforward_down_scale).T
    ffn = jnp.concatenate(
        [feedforward_gate_weight, feedforward_up_weight, down_rows], axis=1
    ).astype(BF16)

    blocks = over_z(over_y(mixing))
    ffn_blocks = z_then_y(ffn)
    rate = -DECAY_FACTOR * jax.nn.softplus(-channel_decay_parameter)
    count, size = recurrence_gate_weight_blocks.shape[:2]
    mix_terms = call(
        recurrence_kernel,
        place,
        (
            gather_features(tokens),
            mixing_norm_gain.reshape(4, -1),
            *blocks,
            recurrent_input_scale.reshape(1, -1),
            convolution_kernel_taps,
            recurrence_gate_weight_blocks,
            input_gate_weight_blocks,
            rate.reshape(1, -1),
            token_extra_log_decay.reshape(-1, 1),
        ),
        rows,
        features,
        [
            pltpu.VMEM((rows + 8, width), F32),
            pltpu.VMEM((count, rows, size), F32),
            pltpu.VMEM((count, rows, size), F32),
        ],
        4 * rows * width * features * 8,
    )
    mixed = (tokens.astype(F32) + share_sums(mix_terms)).astype(BF16)
    hidden_width = feedforward_gate_weight.shape[1]
    down_terms = call(
        ffn_kernel,
        place,
        (
            gather_features(mixed),
            feedforward_norm_gain.reshape(4, -1),
            ffn_blocks,
            feedforward_gate_scale.reshape(1, -1),
            feedforward_up_scale.reshape(1, -1),
        ),
        rows,
        features,
        [],
        6 * rows * hidden_width * features * 8,
    )
    return (mixed.astype(F32) + share_sums(down_terms)).astype(BF16)


def solution(mesh):
    torus = Mesh(
        mesh.devices.reshape(mesh.shape["rep"], 4, 8, 4, 2), ("rep", "z", "y", "x", "c")
    )
    return jax.shard_map(
        body,
        mesh=torus,
        in_specs=(
            P(REP_FS, TP),
            P(),
            P(FS, TP),
            P(TP),
            P(None, TP),
            P(TP, None, None),
            P(TP, None, None),
            P(TP),
            P(REP_FS),
            P(TP, FS),
            P(FS),
            P(),
            P(FS, TP),
            P(TP),
            P(FS, TP),
            P(TP),
            P(TP, FS),
            P(FS),
        ),
        out_specs=P(REP_FS, TP),
        check_vma=False,
    )
```

```python
import jax
import jax.numpy as jnp
from jax import lax
from jax.experimental import pallas as pl
from jax.experimental.pallas import tpu as pltpu
from jax.sharding import Mesh
from jax.sharding import PartitionSpec as P

FS = ("z", "y")
TP = ("x", "c")
REP_FS = ("rep", "z", "y")
EPS = 1e-06
DECAY_FACTOR = 8.0
CHUNKS = 8
F32 = jnp.float32
BF16 = jnp.bfloat16


def shift_z(value, step):
    count = lax.axis_size("rep") * lax.axis_size("z")
    return lax.ppermute(value, ("rep", "z"), [(i, (i + step) % count) for i in range(count)])


def swap(value, axis):
    return lax.all_to_all(value, axis, split_axis=0, concat_axis=0, tiled=True)


def copies_to(value, axis):
    return swap(jnp.broadcast_to(value, (lax.axis_size(axis), *value.shape)), axis)


def to_partner(value):
    return lax.ppermute(value, "c", [(0, 1), (1, 0)])


def chips_in_order(block):
    return copies_to(block, "x")


def share_sums(kept, sent):
    pair = (kept.astype(F32) + to_partner(sent).astype(F32)).astype(BF16)
    return swap(pair, "x").astype(F32).sum(axis=0)


def over_z(own):
    before = shift_z(own, 1)
    after = shift_z(own, -1)
    half = own.shape[0] // 2
    far_low = shift_z(after[:half], -1)
    far_high = shift_z(before[half:], 1)
    return own, before, after, far_low, far_high


def over_y(piece):
    return copies_to(piece, "y").reshape(-1, piece.shape[1])


def gather(piece, axes):
    return lax.all_gather(piece, axes, axis=0, tiled=True)


def z_then_y(piece):
    near = (piece, shift_z(piece, 1), shift_z(piece, -1), shift_z(piece, 2))
    joined = jnp.concatenate(near, axis=1)
    return gather(joined, "y")


def dot(a, b):
    return jnp.dot(a, b, preferred_element_type=F32)


def dot_t(a, b):
    return lax.dot_general(a, b, (((1,), (1,)), ((), ())), preferred_element_type=F32)


def normalize(blocks, gain_ref, normed_ref):
    total = None
    for block, _, _ in blocks:
        v = block[...].astype(F32)
        part = jnp.sum(v * v, axis=-1, keepdims=True)
        total = part if total is None else total + part
    inverse = lax.rsqrt(total / (len(blocks) * blocks[0][0].shape[1]) + EPS)
    for block, x, c in blocks:
        v = block[...].astype(F32)
        normed_ref[x, c] = (v * inverse * gain_ref[x, c]).astype(BF16)


def halves(normed_ref, chip):
    return jnp.concatenate([normed_ref[chip, 0], normed_ref[chip, 1]], axis=1)


def recurrence_kernel(
    place_ref,
    rows_ref,
    partner_ref,
    gain_ref,
    own_ref,
    before_ref,
    after_ref,
    far_low_ref,
    far_high_ref,
    scale_ref,
    taps_ref,
    recur_ref,
    input_ref,
    rate_ref,
    extra_ref,
    kept_ref,
    sent_ref,
    normed_ref,
    padded_ref,
    decay_ref,
    value_ref,
):
    rows = rows_ref.shape[1]
    width = scale_ref.shape[1]
    core = place_ref[0]
    own, before, after, far = (place_ref[i] for i in range(1, 5))
    blocks = [(rows_ref.at[i], i, core) for i in range(rows_ref.shape[0])]
    blocks += [(partner_ref.at[i], i, 1 - core) for i in range(rows_ref.shape[0])]
    normalize(blocks, gain_ref, normed_ref)
    total = dot(halves(normed_ref, own), own_ref[:, :width])
    total += dot(halves(normed_ref, before), before_ref[:, :width])
    total += dot(halves(normed_ref, after), after_ref[:, :width])
    total += dot(normed_ref[far, 0], far_low_ref[:, :width])
    total += dot(normed_ref[far, 1], far_high_ref[:, :width])
    taps = taps_ref.shape[0]
    padded_ref[0:8, :] = jnp.zeros((8, width), F32)
    padded_ref[8:, :] = (total * scale_ref[...]).astype(BF16).astype(F32)
    conv = None
    for k in range(taps):
        start = 8 - (taps - 1) + k
        term = taps_ref[k : k + 1, :] * padded_ref[start : start + rows, :]
        conv = term if conv is None else conv + term
    low = conv.astype(BF16)
    size = recur_ref.shape[1]
    for n in range(recur_ref.shape[0]):
        cols = slice(n * size, (n + 1) * size)
        gate = jax.nn.sigmoid(dot(low[:, cols], recur_ref[n]))
        chosen = jax.nn.sigmoid(dot(low[:, cols], input_ref[n]))
        logarithm = gate * rate_ref[:, cols] + extra_ref[...]
        decay = jnp.exp(logarithm)
        rest = jnp.tanh(-logarithm) * (1.0 + decay * decay)
        decay_ref[n] = decay
        value_ref[n] = jnp.sqrt(rest) * chosen * conv[:, cols]
    count = recur_ref.shape[0]
    steps = rows // CHUNKS

    def step(t, carry):
        new = []
        for n in range(count):
            at = (n, pl.ds(t, CHUNKS, stride=steps), slice(None))
            decay = decay_ref[at]
            state = decay * carry[2 * n] + value_ref[at]
            product = decay * carry[2 * n + 1]
            value_ref[at] = state
            decay_ref[at] = product
            new += [state, product]
        return tuple(new)

    first = (jnp.zeros((CHUNKS, size), F32), jnp.ones((CHUNKS, size), F32)) * count
    ends = lax.fori_loop(0, steps, step, first, unroll=8)
    states = []
    for n in range(count):
        state, product = ends[2 * n], ends[2 * n + 1]
        enter = jnp.zeros((1, size), F32)
        pieces = []
        for chunk in range(CHUNKS):
            span = slice(chunk * steps, (chunk + 1) * steps)
            pieces.append((value_ref[n, span, :] + decay_ref[n, span, :] * enter).astype(BF16))
            enter = state[chunk : chunk + 1] + product[chunk : chunk + 1] * enter
        states.append(jnp.concatenate(pieces, axis=0))
    low = jnp.concatenate(states, axis=1)
    outs = (core, kept_ref, sent_ref)
    store(outs, own, dot_t(low, own_ref[:, width:]))
    store(outs, before, dot_t(low, before_ref[:, width:]))
    store(outs, after, dot_t(low, after_ref[:, width:]))
    low_part = dot_t(low, far_low_ref[:, width:])
    high_part = dot_t(low, far_high_ref[:, width:])
    store(outs, far, jnp.concatenate([low_part, high_part], axis=1))


def store(outs, place, product):
    core, kept_ref, sent_ref = outs
    width = kept_ref.shape[2]
    first = product[:, :width].astype(BF16)
    second = product[:, width:].astype(BF16)
    kept_ref[place] = jnp.where(core == 0, first, second)
    sent_ref[place] = jnp.where(core == 0, second, first)


def ffn_kernel(
    place_ref,
    rows_ref,
    partner_ref,
    gain_ref,
    weights_ref,
    gate_scale_ref,
    up_scale_ref,
    kept_ref,
    sent_ref,
    normed_ref,
):
    core = place_ref[0]
    places = [place_ref[i] for i in range(1, 5)]
    blocks = [(rows_ref.at[i], i, core) for i in range(rows_ref.shape[0])]
    blocks += [(partner_ref.at[i], i, 1 - core) for i in range(rows_ref.shape[0])]
    normalize(blocks, gain_ref, normed_ref)
    width = gate_scale_ref.shape[1]
    total = None
    for k in range(4):
        start = 3 * k * width
        part = dot(halves(normed_ref, places[k]), weights_ref[:, start : start + 2 * width])
        total = part if total is None else total + part
    gate = total[:, :width] * gate_scale_ref[...]
    up = total[:, width:] * up_scale_ref[...]
    hidden = (gate * jax.nn.sigmoid(gate) * up).astype(BF16)
    outs = (core, kept_ref, sent_ref)
    for k in range(4):
        start = (3 * k + 2) * width
        store(outs, places[k], dot_t(hidden, weights_ref[:, start : start + width]))


def call(kernel, place, args, rows, width, scratch, flops):
    vmem = pl.BlockSpec(memory_space=pltpu.VMEM)
    return pl.pallas_call(
        kernel,
        out_shape=[jax.ShapeDtypeStruct((4, rows, width), BF16)] * 2,
        in_specs=[pl.BlockSpec(memory_space=pltpu.SMEM)] + [vmem] * len(args),
        out_specs=[vmem, vmem],
        scratch_shapes=[pltpu.VMEM((4, 2, rows, width), BF16)] + scratch,
        compiler_params=pltpu.CompilerParams(vmem_limit_bytes=56 * 1024 * 1024),
        cost_estimate=pl.CostEstimate(flops=flops, transcendentals=0, bytes_accessed=0),
    )(place, *args)


def layer(
    tokens,
    mixing_norm_gain,
    recurrent_input_weight,
    recurrent_input_scale,
    convolution_kernel_taps,
    recurrence_gate_weight_blocks,
    input_gate_weight_blocks,
    channel_decay_parameter,
    token_extra_log_decay,
    mixing_output_weight,
    mixing_output_scale,
    feedforward_norm_gain,
    feedforward_gate_weight,
    feedforward_gate_scale,
    feedforward_up_weight,
    feedforward_up_scale,
    feedforward_down_weight,
    feedforward_down_scale,
):
    rows, features = tokens.shape
    width = recurrent_input_weight.shape[1]
    z_count = lax.axis_size("z")
    z = lax.axis_index("z")
    near = jnp.array([0, 3, 1, 2], jnp.int32)
    place = jnp.concatenate([lax.axis_index("c")[None], (z + near) % z_count])

    mix_rows = (mixing_output_weight * mixing_output_scale).T
    mixing = jnp.concatenate([recurrent_input_weight, mix_rows], axis=1).astype(BF16)
    down = (feedforward_down_weight * feedforward_down_scale).T
    ffn = jnp.concatenate([feedforward_gate_weight, feedforward_up_weight, down], axis=1)
    ffn = ffn.astype(BF16)

    blocks = over_z(over_y(mixing))
    ffn_blocks = z_then_y(ffn)
    rate = -DECAY_FACTOR * jax.nn.softplus(-channel_decay_parameter)
    count, size = recurrence_gate_weight_blocks.shape[:2]
    tok = chips_in_order(tokens)
    mix_terms = call(
        recurrence_kernel,
        place,
        (
            tok,
            to_partner(tok),
            mixing_norm_gain.reshape(4, 2, 1, -1),
            *blocks,
            recurrent_input_scale.reshape(1, -1),
            convolution_kernel_taps,
            recurrence_gate_weight_blocks,
            input_gate_weight_blocks,
            rate.reshape(1, -1),
            token_extra_log_decay.reshape(-1, 1),
        ),
        rows,
        features,
        [
            pltpu.VMEM((rows + 8, width), F32),
            pltpu.VMEM((count, rows, size), F32),
            pltpu.VMEM((count, rows, size), F32),
        ],
        4 * rows * width * features * 8,
    )
    mixed = (tokens.astype(F32) + share_sums(*mix_terms)).astype(BF16)
    mid = chips_in_order(mixed)
    hidden_width = feedforward_gate_weight.shape[1]
    down_terms = call(
        ffn_kernel,
        place,
        (
            mid,
            to_partner(mid),
            feedforward_norm_gain.reshape(4, 2, 1, -1),
            ffn_blocks,
            feedforward_gate_scale.reshape(1, -1),
            feedforward_up_scale.reshape(1, -1),
        ),
        rows,
        features,
        [],
        6 * rows * hidden_width * features * 8,
    )
    return (mixed.astype(F32) + share_sums(*down_terms)).astype(BF16)


def solution(mesh):
    torus = Mesh(
        mesh.devices.reshape(mesh.shape["rep"], 4, 8, 4, 2), ("rep", "z", "y", "x", "c")
    )
    return jax.shard_map(
        layer,
        mesh=torus,
        in_specs=(
            P(REP_FS, TP),
            P(),
            P(FS, TP),
            P(TP),
            P(None, TP),
            P(TP, None, None),
            P(TP, None, None),
            P(TP),
            P(REP_FS),
            P(TP, FS),
            P(FS),
            P(),
            P(FS, TP),
            P(TP),
            P(FS, TP),
            P(TP),
            P(TP, FS),
            P(FS),
        ),
        out_specs=P(REP_FS, TP),
        check_vma=False,
    )
```

```python
import jax
import jax.numpy as jnp
from jax import lax
from jax.experimental import pallas as pl
from jax.experimental.pallas import tpu as pltpu
from jax.sharding import Mesh
from jax.sharding import PartitionSpec as P

FS = ("z", "y")
TP = ("x", "c")
REP_FS = ("rep", "z", "y")
EPS = 1e-06
DECAY_FACTOR = 8.0
CHUNKS = 8
PIECES = 4
F32 = jnp.float32
BF16 = jnp.bfloat16


def shift_z(value, step):
    count = lax.axis_size("rep") * lax.axis_size("z")
    return lax.ppermute(value, ("rep", "z"), [(i, (i + step) % count) for i in range(count)])


def swap(value, axis):
    return lax.all_to_all(value, axis, split_axis=0, concat_axis=0, tiled=True)


def copies_to(value, axis):
    return swap(jnp.broadcast_to(value, (lax.axis_size(axis), *value.shape)), axis)


def to_partner(value):
    return lax.ppermute(value, "c", [(0, 1), (1, 0)])


def chips_in_order(block):
    return copies_to(block, "x")


def shift_x(value, step):
    count = lax.axis_size("x")
    return lax.ppermute(value, "x", [(i, (i + step) % count) for i in range(count)])


def chips_from_here(block):
    far = shift_x(block, 2)
    near = (block, shift_x(block, 1), shift_x(block, -1), far)
    return jnp.stack(near)


def share_sums(kept, sent):
    pair = (kept.astype(F32) + to_partner(sent).astype(F32)).astype(BF16)
    return swap(pair, "x").astype(F32).sum(axis=0)


def over_z(own, step):
    before = shift_z(own, 1)
    after = shift_z(own, -1)
    far = shift_z(before if step > 0 else after, step)
    return own, before, after, far


def over_plane(mine, other):
    piece = jnp.where(lax.axis_index("rep") == 0, mine, other).astype(BF16)
    return lax.all_gather(piece, ("rep", *FS), axis=0, tiled=True)


def dot(a, b):
    return jnp.dot(a, b, preferred_element_type=F32)


def dot_t(a, b):
    return lax.dot_general(a, b, (((1,), (1,)), ((), ())), preferred_element_type=F32)


def normalize(blocks, gain_ref, normed_ref):
    width = blocks[0][0].shape[1]
    total = None
    for block, _, _ in blocks:
        v = block[...].astype(F32)
        square = v * v
        for start in range(0, width, 128):
            part = square[:, start : start + 128]
            total = part if total is None else total + part
    mean = jnp.sum(total, axis=-1, keepdims=True) / (len(blocks) * width)
    inverse = lax.rsqrt(mean + EPS)
    for block, x, c in blocks:
        v = block[...].astype(F32)
        normed_ref[x, c] = (v * inverse * gain_ref[x, c]).astype(BF16)


def halves(normed_ref, chip):
    return jnp.concatenate([normed_ref[chip, 0], normed_ref[chip, 1]], axis=1)


def nearby(axis):
    here = lax.axis_index(axis)
    return [lax.rem(here + step, 4) for step in (0, 3, 1, 2)]


def recurrence_kernel(
    rows_ref,
    partner_ref,
    gain_ref,
    own_ref,
    before_ref,
    after_ref,
    far_ref,
    scale_ref,
    taps_ref,
    recur_ref,
    input_ref,
    rate_ref,
    extra_ref,
    state_ref,
    normed_ref,
    padded_ref,
    decay_ref,
    value_ref,
):
    rows = rows_ref.shape[1]
    width = own_ref.shape[1]
    core = lax.axis_index("c")
    chips = nearby("x")
    blocks = [(rows_ref.at[i], chip, core) for i, chip in enumerate(chips)]
    blocks += [(partner_ref.at[i], chip, 1 - core) for i, chip in enumerate(chips)]
    normalize(blocks, gain_ref, normed_ref)
    total = None
    for place, ref in zip(nearby("z"), (own_ref, before_ref, after_ref, far_ref)):
        part = dot(halves(normed_ref, place), ref[...])
        total = part if total is None else total + part
    taps = taps_ref.shape[0]
    padded_ref[0:8, :] = jnp.zeros((8, width), F32)
    padded_ref[8:, :] = (total * lanes(scale_ref)).astype(BF16).astype(F32)
    conv = None
    for k in range(taps):
        start = 8 - (taps - 1) + k
        term = taps_ref[k : k + 1, :] * padded_ref[start : start + rows, :]
        conv = term if conv is None else conv + term
    low = conv.astype(BF16)
    size = recur_ref.shape[1]
    extra = [
        jnp.broadcast_to(extra_ref[i], (size, size)).T for i in range(extra_ref.shape[0])
    ]
    extra = jnp.concatenate(extra, axis=0)
    for n in range(recur_ref.shape[0]):
        cols = slice(n * size, (n + 1) * size)
        gate = jax.nn.sigmoid(dot(low[:, cols], recur_ref[n]))
        chosen = jax.nn.sigmoid(dot(low[:, cols], input_ref[n]))
        logarithm = gate * rate_ref[n] + extra
        decay = jnp.exp(logarithm)
        rest = jnp.tanh(-logarithm) * (1.0 + decay * decay)
        decay_ref[n] = decay
        value_ref[n] = jnp.sqrt(rest) * chosen * conv[:, cols]
    count = recur_ref.shape[0]
    steps = rows // CHUNKS

    def step(t, carry):
        new = []
        for n in range(count):
            at = (n, pl.ds(t, CHUNKS, stride=steps), slice(None))
            decay = decay_ref[at]
            state = decay * carry[2 * n] + value_ref[at]
            product = decay * carry[2 * n + 1]
            value_ref[at] = state
            decay_ref[at] = product
            new += [state, product]
        return tuple(new)

    first = (jnp.zeros((CHUNKS, size), F32), jnp.ones((CHUNKS, size), F32)) * count
    ends = lax.fori_loop(0, steps, step, first, unroll=8)
    for n in range(count):
        state, product = ends[2 * n], ends[2 * n + 1]
        cols = slice(n * size, (n + 1) * size)
        enter = jnp.zeros((1, size), F32)
        for chunk in range(CHUNKS):
            span = slice(chunk * steps, (chunk + 1) * steps)
            whole = value_ref[n, span, :] + decay_ref[n, span, :] * enter
            state_ref[span, cols] = whole.astype(BF16)
            enter = state[chunk : chunk + 1] + product[chunk : chunk + 1] * enter


def mixing_kernel(
    state_ref,
    own_ref,
    before_ref,
    after_ref,
    far_ref,
    kept_hbm,
    sent_hbm,
    kept_ref,
    sent_ref,
    sems,
):
    out = Parts(kept_hbm, sent_hbm, kept_ref, sent_ref, sems)
    low = state_ref[...]
    for place, ref in zip(nearby("z"), (own_ref, before_ref, after_ref, far_ref)):
        out.put(place, lambda span: dot_t(low, ref[span, :]))
    out.wait()


def ffn_kernel(
    rows_ref,
    partner_ref,
    gain_ref,
    gate_scale_ref,
    up_scale_ref,
    weights_hbm,
    kept_hbm,
    sent_hbm,
    kept_ref,
    sent_ref,
    out_sems,
    normed_ref,
    in_ref,
    out_ref,
    sems,
):
    width = in_ref.shape[2]
    deep = in_ref.shape[1]
    step = deep // PIECES
    copies = []
    for first, target in ((0, in_ref), (width, out_ref)):
        for side in range(2):
            for piece in range(PIECES):
                span = pl.ds(side * deep + piece * step, step)
                source = weights_hbm.at[span, pl.ds(first, target.shape[2])]
                kept = target.at[side, pl.ds(piece * step, step)]
                copy = pltpu.make_async_copy(source, kept, sems.at[len(copies)])
                copy.start()
                copies.append(copy)

    def arrived(group):
        for copy in copies[group * PIECES : (group + 1) * PIECES]:
            copy.wait()

    core = lax.axis_index("c")
    chips = rows_ref.shape[0]
    blocks = [(rows_ref.at[i], i, core) for i in range(chips)]
    blocks += [(partner_ref.at[i], i, 1 - core) for i in range(chips)]
    normalize(blocks, gain_ref, normed_ref)
    left = jnp.concatenate([halves(normed_ref, x) for x in range(chips)], axis=1)
    arrived(0)
    gate = dot(left, in_ref[0]) * lanes(gate_scale_ref)
    arrived(1)
    up = dot(left, in_ref[1]) * lanes(up_scale_ref)
    hidden = (gate * jax.nn.sigmoid(gate) * up).astype(BF16)
    first, second = hidden[:, : width // 2], hidden[:, width // 2 :]
    arrived(2)
    arrived(3)
    span = deep // chips
    out = Parts(kept_hbm, sent_hbm, kept_ref, sent_ref, out_sems)
    for x in range(chips):

        def product(rows):
            one = dot_t(first, out_ref[0, rows])
            return one + dot_t(second, out_ref[1, rows])

        out.put(x, product, x * span)
    out.wait()


def lanes(ref):
    return jnp.concatenate([ref[n] for n in range(ref.shape[0])], axis=1)


class Parts:
    def __init__(self, kept_hbm, sent_hbm, kept_ref, sent_ref, sems):
        core = lax.axis_index("c")
        self.sides = ((core, kept_ref, kept_hbm), (1 - core, sent_ref, sent_hbm))
        self.width = kept_ref.shape[2]
        self.sems = sems
        self.copies = []

    def put(self, place, product, base=0):
        for half, ref, out in self.sides:
            start = pl.multiple_of(base + half * self.width, self.width)
            ref[place] = product(pl.ds(start, self.width)).astype(BF16)
            sem = self.sems.at[len(self.copies)]
            copy = pltpu.make_async_copy(ref.at[place], out.at[place], sem)
            copy.start()
            self.copies.append(copy)

    def wait(self):
        for copy in self.copies:
            copy.wait()


def call(kernel, small, large, outs, scratch, flops):
    vmem = pl.BlockSpec(memory_space=pltpu.VMEM)
    hbm = pl.BlockSpec(memory_space=pl.ANY)
    out_specs = [vmem]
    if len(outs) > 1:
        out_specs = [hbm] * len(outs)
        scratch = [pltpu.VMEM(shape, BF16) for shape in outs] + [
            pltpu.SemaphoreType.DMA((8,)),
            *scratch,
        ]
    return pl.pallas_call(
        kernel,
        out_shape=[jax.ShapeDtypeStruct(shape, BF16) for shape in outs],
        in_specs=[vmem] * len(small) + [hbm] * len(large),
        out_specs=out_specs,
        scratch_shapes=scratch,
        compiler_params=pltpu.CompilerParams(vmem_limit_bytes=56 * 1024 * 1024),
        cost_estimate=pl.CostEstimate(flops=flops, transcendentals=0, bytes_accessed=0),
    )(*small, *large)


def layer(
    tokens,
    mixing_norm_gain,
    recurrent_input_weight,
    recurrent_input_scale,
    convolution_kernel_taps,
    recurrence_gate_weight_blocks,
    input_gate_weight_blocks,
    channel_decay_parameter,
    token_extra_log_decay,
    mixing_output_weight,
    mixing_output_scale,
    feedforward_norm_gain,
    feedforward_gate_weight,
    feedforward_gate_scale,
    feedforward_up_weight,
    feedforward_up_scale,
    feedforward_down_weight,
    feedforward_down_scale,
):
    rows, features = tokens.shape
    width = recurrent_input_weight.shape[1]
    mix_rows = (mixing_output_weight * mixing_output_scale).T
    pair = jnp.stack([recurrent_input_weight, mix_rows]).astype(BF16)
    down = (feedforward_down_weight * feedforward_down_scale).T
    half = down.shape[1] // 2
    ffn_blocks = over_plane(
        jnp.concatenate([feedforward_gate_weight, down[:, :half]], axis=1),
        jnp.concatenate([feedforward_up_weight, down[:, half:]], axis=1),
    )

    pair = copies_to(pair, "y")
    rec_blocks = over_z(pair[:, 0].reshape(-1, width), 1)
    mix_blocks = over_z(pair[:, 1].reshape(-1, width), -1)
    rate = -DECAY_FACTOR * jax.nn.softplus(-channel_decay_parameter)
    count, size = recurrence_gate_weight_blocks.shape[:2]
    tok = chips_from_here(tokens)
    terms = [(4, rows, features)] * 2
    normed = pltpu.VMEM((4, 2, rows, features), BF16)
    (state,) = call(
        recurrence_kernel,
        (
            tok,
            to_partner(tok),
            mixing_norm_gain.reshape(4, 2, 1, -1),
            *rec_blocks,
            recurrent_input_scale.reshape(-1, 1, size),
            convolution_kernel_taps,
            recurrence_gate_weight_blocks,
            input_gate_weight_blocks,
            rate.reshape(-1, 1, size),
            token_extra_log_decay.reshape(-1, 1, size),
        ),
        (),
        [(rows, width)],
        [
            normed,
            pltpu.VMEM((rows + 8, width), F32),
            pltpu.VMEM((count, rows, size), F32),
            pltpu.VMEM((count, rows, size), F32),
        ],
        2 * rows * width * features * 8,
    )
    mix_terms = call(
        mixing_kernel,
        (state, *mix_blocks),
        (),
        terms,
        [],
        2 * rows * width * features * 8,
    )
    mixed = (tokens.astype(F32) + share_sums(*mix_terms)).astype(BF16)
    mid = chips_in_order(mixed)
    hidden_width = feedforward_gate_weight.shape[1]
    down_terms = call(
        ffn_kernel,
        (
            mid,
            to_partner(mid),
            feedforward_norm_gain.reshape(4, 2, 1, -1),
            feedforward_gate_scale.reshape(-1, 1, size),
            feedforward_up_scale.reshape(-1, 1, size),
        ),
        (ffn_blocks,),
        terms,
        [
            normed,
            pltpu.VMEM((2, 8 * features, hidden_width), BF16),
            pltpu.VMEM((2, 8 * features, hidden_width // 2), BF16),
            pltpu.SemaphoreType.DMA((4 * PIECES,)),
        ],
        6 * rows * hidden_width * features * 8,
    )
    return (mixed.astype(F32) + share_sums(*down_terms)).astype(BF16)


def solution(mesh):
    torus = Mesh(
        mesh.devices.reshape(mesh.shape["rep"], 4, 8, 4, 2), ("rep", "z", "y", "x", "c")
    )
    return jax.shard_map(
        layer,
        mesh=torus,
        in_specs=(
            P(REP_FS, TP),
            P(),
            P(FS, TP),
            P(TP),
            P(None, TP),
            P(TP, None, None),
            P(TP, None, None),
            P(TP),
            P(REP_FS),
            P(TP, FS),
            P(FS),
            P(),
            P(FS, TP),
            P(TP),
            P(FS, TP),
            P(TP),
            P(TP, FS),
            P(FS),
        ),
        out_specs=P(REP_FS, TP),
        check_vma=False,
    )
```

```python
import jax
import jax.numpy as jnp
from jax import lax
from jax.experimental import pallas as pl
from jax.experimental.pallas import tpu as pltpu
from jax.sharding import Mesh
from jax.sharding import PartitionSpec as P

FS = ("z", "y")
TP = ("x", "c")
REP_FS = ("rep", "z", "y")
EPS = 1e-06
DECAY_FACTOR = 8.0
CHUNKS = 8
PIECES = 4
F32 = jnp.float32
BF16 = jnp.bfloat16


def shift_z(value, step):
    count = lax.axis_size("rep") * lax.axis_size("z")
    return lax.ppermute(value, ("rep", "z"), [(i, (i + step) % count) for i in range(count)])


def swap(value, axis):
    return lax.all_to_all(value, axis, split_axis=0, concat_axis=0, tiled=True)


def copies_to(value, axis):
    return swap(jnp.broadcast_to(value, (lax.axis_size(axis), *value.shape)), axis)


def to_partner(value):
    return lax.ppermute(value, "c", [(0, 1), (1, 0)])


def chips_in_order(block):
    return copies_to(block, "x")


def shift_x(value, step):
    count = lax.axis_size("x")
    return lax.ppermute(value, "x", [(i, (i + step) % count) for i in range(count)])


def chips_from_here(block):
    far = shift_x(block, 2)
    near = (block, shift_x(block, 1), shift_x(block, -1), far)
    return jnp.stack(near)


def share_sums(kept, sent):
    pair = (kept.astype(F32) + to_partner(sent).astype(F32)).astype(BF16)
    return swap(pair, "x").astype(F32).sum(axis=0)


def over_z(own, step):
    before = shift_z(own, 1)
    after = shift_z(own, -1)
    far = shift_z(before if step > 0 else after, step)
    return own, before, after, far


def over_plane(mine, other):
    piece = jnp.where(lax.axis_index("rep") == 0, mine, other).astype(BF16)
    return lax.all_gather(piece, ("rep", *FS), axis=0, tiled=True)


def dot(a, b):
    return jnp.dot(a, b, preferred_element_type=F32)


def dot_t(a, b):
    return lax.dot_general(a, b, (((1,), (1,)), ((), ())), preferred_element_type=F32)


def normalize(blocks, gain_ref, normed_ref):
    width = blocks[0][0].shape[1]
    total = None
    for block, _, _ in blocks:
        v = block[...].astype(F32)
        square = v * v
        for start in range(0, width, 128):
            part = square[:, start : start + 128]
            total = part if total is None else total + part
    mean = jnp.sum(total, axis=-1, keepdims=True) / (len(blocks) * width)
    inverse = lax.rsqrt(mean + EPS)
    for block, x, c in blocks:
        v = block[...].astype(F32)
        normed_ref[x, c] = (v * inverse * gain_ref[x, c]).astype(BF16)


def halves(normed_ref, chip):
    return jnp.concatenate([normed_ref[chip, 0], normed_ref[chip, 1]], axis=1)


def pack_kernel(rec_ref, mix_ref, scale_ref, out_hbm, both_ref, sems):
    both_ref[0] = rec_ref[...].astype(BF16)
    rows = mix_ref.shape[0]
    scale = jnp.concatenate([scale_ref[...]] * (128 // rows), axis=1)
    column = jnp.broadcast_to(scale, (128, 128)).T[:rows, :1]
    both_ref[1] = (mix_ref[...] * column).astype(BF16)
    copies = [
        pltpu.make_async_copy(both_ref, out_hbm.at[i], sems.at[i]) for i in range(out_hbm.shape[0])
    ]
    for copy in copies:
        copy.start()
    for copy in copies:
        copy.wait()


def pack(rec, mix, scale, count):
    rows, width = rec.shape
    vmem = pl.BlockSpec(memory_space=pltpu.VMEM)
    return pl.pallas_call(
        pack_kernel,
        out_shape=jax.ShapeDtypeStruct((count, 2, rows, width), BF16),
        in_specs=[vmem] * 3,
        out_specs=pl.BlockSpec(memory_space=pl.ANY),
        scratch_shapes=[pltpu.VMEM((2, rows, width), BF16), pltpu.SemaphoreType.DMA((count,))],
    )(rec, mix.T, scale.reshape(1, rows))


def nearby(axis):
    here = lax.axis_index(axis)
    return [lax.rem(here + step, 4) for step in (0, 3, 1, 2)]


def recurrence_kernel(
    rows_ref,
    partner_ref,
    gain_ref,
    own_ref,
    before_ref,
    after_ref,
    far_ref,
    scale_ref,
    taps_ref,
    recur_ref,
    input_ref,
    rate_ref,
    extra_ref,
    state_ref,
    normed_ref,
    padded_ref,
    decay_ref,
    value_ref,
):
    rows = rows_ref.shape[1]
    width = own_ref.shape[1]
    core = lax.axis_index("c")
    chips = nearby("x")
    blocks = [(rows_ref.at[i], chip, core) for i, chip in enumerate(chips)]
    blocks += [(partner_ref.at[i], chip, 1 - core) for i, chip in enumerate(chips)]
    normalize(blocks, gain_ref, normed_ref)
    total = None
    for place, ref in zip(nearby("z"), (own_ref, before_ref, after_ref, far_ref)):
        part = dot(halves(normed_ref, place), ref[...])
        total = part if total is None else total + part
    taps = taps_ref.shape[0]
    padded_ref[0:8, :] = jnp.zeros((8, width), F32)
    padded_ref[8:, :] = (total * lanes(scale_ref)).astype(BF16).astype(F32)
    conv = None
    for k in range(taps):
        start = 8 - (taps - 1) + k
        term = taps_ref[k : k + 1, :] * padded_ref[start : start + rows, :]
        conv = term if conv is None else conv + term
    low = conv.astype(BF16)
    size = recur_ref.shape[1]
    extra = [
        jnp.broadcast_to(extra_ref[i], (size, size)).T for i in range(extra_ref.shape[0])
    ]
    extra = jnp.concatenate(extra, axis=0)
    for n in range(recur_ref.shape[0]):
        cols = slice(n * size, (n + 1) * size)
        gate = jax.nn.sigmoid(dot(low[:, cols], recur_ref[n]))
        chosen = jax.nn.sigmoid(dot(low[:, cols], input_ref[n]))
        logarithm = gate * rate_ref[n] + extra
        decay = jnp.exp(logarithm)
        rest = jnp.tanh(-logarithm) * (1.0 + decay * decay)
        decay_ref[n] = decay
        value_ref[n] = jnp.sqrt(rest) * chosen * conv[:, cols]
    count = recur_ref.shape[0]
    steps = rows // CHUNKS

    def step(t, carry):
        new = []
        for n in range(count):
            at = (n, pl.ds(t, CHUNKS, stride=steps), slice(None))
            decay = decay_ref[at]
            state = decay * carry[2 * n] + value_ref[at]
            product = decay * carry[2 * n + 1]
            value_ref[at] = state
            decay_ref[at] = product
            new += [state, product]
        return tuple(new)

    first = (jnp.zeros((CHUNKS, size), F32), jnp.ones((CHUNKS, size), F32)) * count
    ends = lax.fori_loop(0, steps, step, first, unroll=8)
    for n in range(count):
        state, product = ends[2 * n], ends[2 * n + 1]
        cols = slice(n * size, (n + 1) * size)
        enter = jnp.zeros((1, size), F32)
        for chunk in range(CHUNKS):
            span = slice(chunk * steps, (chunk + 1) * steps)
            whole = value_ref[n, span, :] + decay_ref[n, span, :] * enter
            state_ref[span, cols] = whole.astype(BF16)
            enter = state[chunk : chunk + 1] + product[chunk : chunk + 1] * enter


def mixing_kernel(
    state_ref,
    own_ref,
    before_ref,
    after_ref,
    far_ref,
    kept_hbm,
    sent_hbm,
    kept_ref,
    sent_ref,
    sems,
):
    out = Parts(kept_hbm, sent_hbm, kept_ref, sent_ref, sems)
    low = state_ref[...]
    for place, ref in zip(nearby("z"), (own_ref, before_ref, after_ref, far_ref)):
        out.put(place, lambda span: dot_t(low, ref[span, :]))
    out.wait()


def ffn_kernel(
    rows_ref,
    partner_ref,
    gain_ref,
    gate_scale_ref,
    up_scale_ref,
    weights_hbm,
    kept_hbm,
    sent_hbm,
    kept_ref,
    sent_ref,
    out_sems,
    normed_ref,
    weights_ref,
    sems,
):
    width = 128 * gate_scale_ref.shape[0]
    deep = weights_ref.shape[1]
    step = deep // PIECES
    copies = []
    for side in range(2):
        for piece in range(PIECES):
            source = weights_hbm.at[pl.ds(side * deep + piece * step, step)]
            target = weights_ref.at[side, pl.ds(piece * step, step)]
            copy = pltpu.make_async_copy(source, target, sems.at[len(copies)])
            copy.start()
            copies.append(copy)

    def arrived(side):
        for copy in copies[side * PIECES : (side + 1) * PIECES]:
            copy.wait()

    core = lax.axis_index("c")
    chips = rows_ref.shape[0]
    blocks = [(rows_ref.at[i], i, core) for i in range(chips)]
    blocks += [(partner_ref.at[i], i, 1 - core) for i in range(chips)]
    normalize(blocks, gain_ref, normed_ref)
    left = jnp.concatenate([halves(normed_ref, x) for x in range(chips)], axis=1)
    arrived(0)
    gate = dot(left, weights_ref[0, :, :width]) * lanes(gate_scale_ref)
    arrived(1)
    up = dot(left, weights_ref[1, :, :width]) * lanes(up_scale_ref)
    hidden = (gate * jax.nn.sigmoid(gate) * up).astype(BF16)
    first, second = hidden[:, : width // 2], hidden[:, width // 2 :]
    span = deep // chips
    out = Parts(kept_hbm, sent_hbm, kept_ref, sent_ref, out_sems)
    for x in range(chips):

        def product(rows):
            one = dot_t(first, weights_ref[0, rows, width:])
            return one + dot_t(second, weights_ref[1, rows, width:])

        out.put(x, product, x * span)
    out.wait()


def lanes(ref):
    return jnp.concatenate([ref[n] for n in range(ref.shape[0])], axis=1)


class Parts:
    def __init__(self, kept_hbm, sent_hbm, kept_ref, sent_ref, sems):
        core = lax.axis_index("c")
        self.sides = ((core, kept_ref, kept_hbm), (1 - core, sent_ref, sent_hbm))
        self.width = kept_ref.shape[2]
        self.sems = sems
        self.copies = []

    def put(self, place, product, base=0):
        for half, ref, out in self.sides:
            start = pl.multiple_of(base + half * self.width, self.width)
            ref[place] = product(pl.ds(start, self.width)).astype(BF16)
            sem = self.sems.at[len(self.copies)]
            copy = pltpu.make_async_copy(ref.at[place], out.at[place], sem)
            copy.start()
            self.copies.append(copy)

    def wait(self):
        for copy in self.copies:
            copy.wait()


def call(kernel, small, large, outs, scratch, flops):
    vmem = pl.BlockSpec(memory_space=pltpu.VMEM)
    hbm = pl.BlockSpec(memory_space=pl.ANY)
    out_specs = [vmem]
    if len(outs) > 1:
        out_specs = [hbm] * len(outs)
        scratch = [pltpu.VMEM(shape, BF16) for shape in outs] + [
            pltpu.SemaphoreType.DMA((8,)),
            *scratch,
        ]
    return pl.pallas_call(
        kernel,
        out_shape=[jax.ShapeDtypeStruct(shape, BF16) for shape in outs],
        in_specs=[vmem] * len(small) + [hbm] * len(large),
        out_specs=out_specs,
        scratch_shapes=scratch,
        compiler_params=pltpu.CompilerParams(vmem_limit_bytes=56 * 1024 * 1024),
        cost_estimate=pl.CostEstimate(flops=flops, transcendentals=0, bytes_accessed=0),
    )(*small, *large)


def layer(
    tokens,
    mixing_norm_gain,
    recurrent_input_weight,
    recurrent_input_scale,
    convolution_kernel_taps,
    recurrence_gate_weight_blocks,
    input_gate_weight_blocks,
    channel_decay_parameter,
    token_extra_log_decay,
    mixing_output_weight,
    mixing_output_scale,
    feedforward_norm_gain,
    feedforward_gate_weight,
    feedforward_gate_scale,
    feedforward_up_weight,
    feedforward_up_scale,
    feedforward_down_weight,
    feedforward_down_scale,
):
    rows, features = tokens.shape
    width = recurrent_input_weight.shape[1]
    down = (feedforward_down_weight * feedforward_down_scale).T
    half = down.shape[1] // 2
    ffn_blocks = over_plane(
        jnp.concatenate([feedforward_gate_weight, down[:, :half]], axis=1),
        jnp.concatenate([feedforward_up_weight, down[:, half:]], axis=1),
    )

    copies = pack(
        recurrent_input_weight, mixing_output_weight, mixing_output_scale, lax.axis_size("y")
    )
    pair = swap(copies, "y")
    rec_blocks = over_z(pair[:, 0].reshape(-1, width), 1)
    mix_blocks = over_z(pair[:, 1].reshape(-1, width), -1)
    rate = -DECAY_FACTOR * jax.nn.softplus(-channel_decay_parameter)
    count, size = recurrence_gate_weight_blocks.shape[:2]
    vectors = (recurrent_input_scale, rate, token_extra_log_decay)
    vectors = [v.reshape(-1, 1, size) for v in vectors]
    tok, scale, rate, extra = lax.optimization_barrier((tokens, *vectors))
    tok = chips_from_here(tok)
    terms = [(4, rows, features)] * 2
    normed = pltpu.VMEM((4, 2, rows, features), BF16)
    (state,) = call(
        recurrence_kernel,
        (
            tok,
            to_partner(tok),
            mixing_norm_gain.reshape(4, 2, 1, -1),
            *rec_blocks,
            scale,
            convolution_kernel_taps,
            recurrence_gate_weight_blocks,
            input_gate_weight_blocks,
            rate,
            extra,
        ),
        (),
        [(rows, width)],
        [
            normed,
            pltpu.VMEM((rows + 8, width), F32),
            pltpu.VMEM((count, rows, size), F32),
            pltpu.VMEM((count, rows, size), F32),
        ],
        2 * rows * width * features * 8,
    )
    mix_terms = call(
        mixing_kernel,
        (state, *mix_blocks),
        (),
        terms,
        [],
        2 * rows * width * features * 8,
    )
    mixed = (tokens.astype(F32) + share_sums(*mix_terms)).astype(BF16)
    mid = chips_in_order(mixed)
    hidden_width = feedforward_gate_weight.shape[1]
    down_terms = call(
        ffn_kernel,
        (
            mid,
            to_partner(mid),
            feedforward_norm_gain.reshape(4, 2, 1, -1),
            feedforward_gate_scale.reshape(-1, 1, size),
            feedforward_up_scale.reshape(-1, 1, size),
        ),
        (ffn_blocks,),
        terms,
        [
            normed,
            pltpu.VMEM((2, 8 * features, ffn_blocks.shape[1]), BF16),
            pltpu.SemaphoreType.DMA((2 * PIECES,)),
        ],
        6 * rows * hidden_width * features * 8,
    )
    return (mixed.astype(F32) + share_sums(*down_terms)).astype(BF16)


def solution(mesh):
    torus = Mesh(
        mesh.devices.reshape(mesh.shape["rep"], 4, 8, 4, 2), ("rep", "z", "y", "x", "c")
    )
    return jax.shard_map(
        layer,
        mesh=torus,
        in_specs=(
            P(REP_FS, TP),
            P(),
            P(FS, TP),
            P(TP),
            P(None, TP),
            P(TP, None, None),
            P(TP, None, None),
            P(TP),
            P(REP_FS),
            P(TP, FS),
            P(FS),
            P(),
            P(FS, TP),
            P(TP),
            P(FS, TP),
            P(TP),
            P(TP, FS),
            P(FS),
        ),
        out_specs=P(REP_FS, TP),
        check_vma=False,
    )
```

```python
import jax
import jax.numpy as jnp
from jax import lax
from jax.experimental import pallas as pl
from jax.experimental.pallas import tpu as pltpu
from jax.sharding import Mesh
from jax.sharding import PartitionSpec as P

FS = ("z", "y")
TP = ("x", "c")
REP_FS = ("rep", "z", "y")
EPS = 1e-06
DECAY_FACTOR = 8.0
CHUNKS = 8
PIECES = 4
F32 = jnp.float32
BF16 = jnp.bfloat16


def shift_z(value, step):
    count = lax.axis_size("rep") * lax.axis_size("z")
    return lax.ppermute(value, ("rep", "z"), [(i, (i + step) % count) for i in range(count)])


def swap(value, axis):
    return lax.all_to_all(value, axis, split_axis=0, concat_axis=0, tiled=True)


def copies_to(value, axis):
    return swap(jnp.broadcast_to(value, (lax.axis_size(axis), *value.shape)), axis)


def to_partner(value):
    return lax.ppermute(value, "c", [(0, 1), (1, 0)])


def chips_in_order(block):
    return copies_to(block, "x")


def shift_x(value, step):
    count = lax.axis_size("x")
    return lax.ppermute(value, "x", [(i, (i + step) % count) for i in range(count)])


def chips_from_here(block):
    far = shift_x(block, 2)
    near = (block, shift_x(block, 1), shift_x(block, -1), far)
    return jnp.stack(near)


def share_sums(kept, sent):
    pair = (kept.astype(F32) + to_partner(sent).astype(F32)).astype(BF16)
    return swap(pair, "x").astype(F32).sum(axis=0)


def over_z(own, step):
    before = shift_z(own, 1)
    after = shift_z(own, -1)
    far = shift_z(before if step > 0 else after, step)
    return own, before, after, far


def over_plane(mine, other):
    piece = jnp.where(lax.axis_index("rep") == 0, mine, other).astype(BF16)
    return lax.all_gather(piece, ("rep", *FS), axis=0, tiled=True)


def dot(a, b):
    return jnp.dot(a, b, preferred_element_type=F32)


def dot_t(a, b):
    return lax.dot_general(a, b, (((1,), (1,)), ((), ())), preferred_element_type=F32)


def normalize(blocks, gain_ref, normed_ref):
    width = blocks[0][0].shape[1]
    total = None
    for block, _, _ in blocks:
        v = block[...].astype(F32)
        square = v * v
        for start in range(0, width, 128):
            part = square[:, start : start + 128]
            total = part if total is None else total + part
    mean = jnp.sum(total, axis=-1, keepdims=True) / (len(blocks) * width)
    inverse = lax.rsqrt(mean + EPS)
    for block, x, c in blocks:
        v = block[...].astype(F32)
        normed_ref[x, c] = (v * inverse * gain_ref[x, c]).astype(BF16)


def halves(normed_ref, chip):
    return jnp.concatenate([normed_ref[chip, 0], normed_ref[chip, 1]], axis=1)


def pack_kernel(rec_ref, mix_ref, scale_ref, out_hbm, both_ref, sems):
    both_ref[0] = rec_ref[...].astype(BF16)
    rows = mix_ref.shape[0]
    scale = jnp.concatenate([scale_ref[...]] * (128 // rows), axis=1)
    column = jnp.broadcast_to(scale, (128, 128)).T[:rows, :1]
    both_ref[1] = (mix_ref[...] * column).astype(BF16)
    copies = [
        pltpu.make_async_copy(both_ref, out_hbm.at[i], sems.at[i]) for i in range(out_hbm.shape[0])
    ]
    for copy in copies:
        copy.start()
    for copy in copies:
        copy.wait()


def pack(rec, mix, scale, count):
    rows, width = rec.shape
    vmem = pl.BlockSpec(memory_space=pltpu.VMEM)
    return pl.pallas_call(
        pack_kernel,
        out_shape=jax.ShapeDtypeStruct((count, 2, rows, width), BF16),
        in_specs=[vmem] * 3,
        out_specs=pl.BlockSpec(memory_space=pl.ANY),
        scratch_shapes=[pltpu.VMEM((2, rows, width), BF16), pltpu.SemaphoreType.DMA((count,))],
    )(rec, mix.T, scale.reshape(1, rows))


def nearby(axis):
    here = lax.axis_index(axis)
    return [lax.rem(here + step, 4) for step in (0, 3, 1, 2)]


def recurrence_kernel(
    rows_ref,
    partner_ref,
    gain_ref,
    own_ref,
    before_ref,
    after_ref,
    far_ref,
    scale_ref,
    taps_ref,
    recur_ref,
    input_ref,
    rate_ref,
    extra_ref,
    state_ref,
    normed_ref,
    padded_ref,
    decay_ref,
    value_ref,
):
    rows = rows_ref.shape[1]
    width = own_ref.shape[1]
    core = lax.axis_index("c")
    chips = nearby("x")
    blocks = [(rows_ref.at[i], chip, core) for i, chip in enumerate(chips)]
    blocks += [(partner_ref.at[i], chip, 1 - core) for i, chip in enumerate(chips)]
    normalize(blocks, gain_ref, normed_ref)
    total = None
    for place, ref in zip(nearby("z"), (own_ref, before_ref, after_ref, far_ref)):
        part = dot(halves(normed_ref, place), ref[...])
        total = part if total is None else total + part
    taps = taps_ref.shape[0]
    padded_ref[0:8, :] = jnp.zeros((8, width), F32)
    padded_ref[8:, :] = (total * lanes(scale_ref)).astype(BF16).astype(F32)
    conv = None
    for k in range(taps):
        start = 8 - (taps - 1) + k
        term = taps_ref[k : k + 1, :] * padded_ref[start : start + rows, :]
        conv = term if conv is None else conv + term
    low = conv.astype(BF16)
    size = recur_ref.shape[1]
    extra = [
        jnp.broadcast_to(extra_ref[i], (size, size)).T for i in range(extra_ref.shape[0])
    ]
    extra = jnp.concatenate(extra, axis=0)
    for n in range(recur_ref.shape[0]):
        cols = slice(n * size, (n + 1) * size)
        gate = jax.nn.sigmoid(dot(low[:, cols], recur_ref[n]))
        chosen = jax.nn.sigmoid(dot(low[:, cols], input_ref[n]))
        logarithm = gate * rate_ref[n] + extra
        decay = jnp.exp(logarithm)
        rest = jnp.tanh(-logarithm) * (1.0 + decay * decay)
        decay_ref[n] = decay
        value_ref[n] = jnp.sqrt(rest) * chosen * conv[:, cols]
    count = recur_ref.shape[0]
    steps = rows // CHUNKS

    def step(t, carry):
        new = []
        for n in range(count):
            at = (n, pl.ds(t, CHUNKS, stride=steps), slice(None))
            decay = decay_ref[at]
            state = decay * carry[2 * n] + value_ref[at]
            product = decay * carry[2 * n + 1]
            value_ref[at] = state
            decay_ref[at] = product
            new += [state, product]
        return tuple(new)

    first = (jnp.zeros((CHUNKS, size), F32), jnp.ones((CHUNKS, size), F32)) * count
    ends = lax.fori_loop(0, steps, step, first, unroll=8)
    for n in range(count):
        state, product = ends[2 * n], ends[2 * n + 1]
        cols = slice(n * size, (n + 1) * size)
        enter = jnp.zeros((1, size), F32)
        for chunk in range(CHUNKS):
            span = slice(chunk * steps, (chunk + 1) * steps)
            whole = value_ref[n, span, :] + decay_ref[n, span, :] * enter
            state_ref[span, cols] = whole.astype(BF16)
            enter = state[chunk : chunk + 1] + product[chunk : chunk + 1] * enter


def mixing_kernel(
    state_ref,
    own_ref,
    before_ref,
    after_ref,
    far_ref,
    kept_hbm,
    sent_hbm,
    kept_ref,
    sent_ref,
    sems,
):
    out = Parts(kept_hbm, sent_hbm, kept_ref, sent_ref, sems)
    low = state_ref[...]
    for place, ref in zip(nearby("z"), (own_ref, before_ref, after_ref, far_ref)):
        out.put(place, lambda span: dot_t(low, ref[span, :]))
    out.wait()


def ffn_kernel(
    rows_ref,
    partner_ref,
    gain_ref,
    gate_scale_ref,
    up_scale_ref,
    weights_hbm,
    kept_hbm,
    sent_hbm,
    kept_ref,
    sent_ref,
    out_sems,
    normed_ref,
    in_ref,
    out_ref,
    sems,
):
    width = in_ref.shape[2]
    deep = in_ref.shape[1]
    step = deep // PIECES
    copies = []
    for first, target in ((0, in_ref), (width, out_ref)):
        for side in range(2):
            for piece in range(PIECES):
                span = pl.ds(side * deep + piece * step, step)
                source = weights_hbm.at[span, pl.ds(first, target.shape[2])]
                kept = target.at[side, pl.ds(piece * step, step)]
                copy = pltpu.make_async_copy(source, kept, sems.at[len(copies)])
                copy.start()
                copies.append(copy)

    def arrived(group):
        for copy in copies[group * PIECES : (group + 1) * PIECES]:
            copy.wait()

    core = lax.axis_index("c")
    chips = rows_ref.shape[0]
    blocks = [(rows_ref.at[i], i, core) for i in range(chips)]
    blocks += [(partner_ref.at[i], i, 1 - core) for i in range(chips)]
    normalize(blocks, gain_ref, normed_ref)
    left = jnp.concatenate([halves(normed_ref, x) for x in range(chips)], axis=1)
    arrived(0)
    gate = dot(left, in_ref[0]) * lanes(gate_scale_ref)
    arrived(1)
    up = dot(left, in_ref[1]) * lanes(up_scale_ref)
    hidden = (gate * jax.nn.sigmoid(gate) * up).astype(BF16)
    first, second = hidden[:, : width // 2], hidden[:, width // 2 :]
    arrived(2)
    arrived(3)
    span = deep // chips
    out = Parts(kept_hbm, sent_hbm, kept_ref, sent_ref, out_sems)
    for x in range(chips):

        def product(rows):
            one = dot_t(first, out_ref[0, rows])
            return one + dot_t(second, out_ref[1, rows])

        out.put(x, product, x * span)
    out.wait()


def lanes(ref):
    return jnp.concatenate([ref[n] for n in range(ref.shape[0])], axis=1)


class Parts:
    def __init__(self, kept_hbm, sent_hbm, kept_ref, sent_ref, sems):
        core = lax.axis_index("c")
        self.sides = ((core, kept_ref, kept_hbm), (1 - core, sent_ref, sent_hbm))
        self.width = kept_ref.shape[2]
        self.sems = sems
        self.copies = []

    def put(self, place, product, base=0):
        for half, ref, out in self.sides:
            start = pl.multiple_of(base + half * self.width, self.width)
            ref[place] = product(pl.ds(start, self.width)).astype(BF16)
            sem = self.sems.at[len(self.copies)]
            copy = pltpu.make_async_copy(ref.at[place], out.at[place], sem)
            copy.start()
            self.copies.append(copy)

    def wait(self):
        for copy in self.copies:
            copy.wait()


def call(kernel, small, large, outs, scratch, flops):
    vmem = pl.BlockSpec(memory_space=pltpu.VMEM)
    hbm = pl.BlockSpec(memory_space=pl.ANY)
    out_specs = [vmem]
    if len(outs) > 1:
        out_specs = [hbm] * len(outs)
        scratch = [pltpu.VMEM(shape, BF16) for shape in outs] + [
            pltpu.SemaphoreType.DMA((8,)),
            *scratch,
        ]
    return pl.pallas_call(
        kernel,
        out_shape=[jax.ShapeDtypeStruct(shape, BF16) for shape in outs],
        in_specs=[vmem] * len(small) + [hbm] * len(large),
        out_specs=out_specs,
        scratch_shapes=scratch,
        compiler_params=pltpu.CompilerParams(vmem_limit_bytes=56 * 1024 * 1024),
        cost_estimate=pl.CostEstimate(flops=flops, transcendentals=0, bytes_accessed=0),
    )(*small, *large)


def layer(
    tokens,
    mixing_norm_gain,
    recurrent_input_weight,
    recurrent_input_scale,
    convolution_kernel_taps,
    recurrence_gate_weight_blocks,
    input_gate_weight_blocks,
    channel_decay_parameter,
    token_extra_log_decay,
    mixing_output_weight,
    mixing_output_scale,
    feedforward_norm_gain,
    feedforward_gate_weight,
    feedforward_gate_scale,
    feedforward_up_weight,
    feedforward_up_scale,
    feedforward_down_weight,
    feedforward_down_scale,
):
    rows, features = tokens.shape
    width = recurrent_input_weight.shape[1]
    down = (feedforward_down_weight * feedforward_down_scale).T
    half = down.shape[1] // 2
    ffn_blocks = over_plane(
        jnp.concatenate([feedforward_gate_weight, down[:, :half]], axis=1),
        jnp.concatenate([feedforward_up_weight, down[:, half:]], axis=1),
    )

    copies = pack(
        recurrent_input_weight, mixing_output_weight, mixing_output_scale, lax.axis_size("y")
    )
    pair = swap(copies, "y")
    rec_blocks = over_z(pair[:, 0].reshape(-1, width), 1)
    mix_blocks = over_z(pair[:, 1].reshape(-1, width), -1)
    rate = -DECAY_FACTOR * jax.nn.softplus(-channel_decay_parameter)
    count, size = recurrence_gate_weight_blocks.shape[:2]
    vectors = (recurrent_input_scale, rate, token_extra_log_decay)
    vectors = [v.reshape(-1, 1, size) for v in vectors]
    tok, scale, rate, extra = lax.optimization_barrier((tokens, *vectors))
    tok = chips_from_here(tok)
    terms = [(4, rows, features)] * 2
    normed = pltpu.VMEM((4, 2, rows, features), BF16)
    (state,) = call(
        recurrence_kernel,
        (
            tok,
            to_partner(tok),
            mixing_norm_gain.reshape(4, 2, 1, -1),
            *rec_blocks,
            scale,
            convolution_kernel_taps,
            recurrence_gate_weight_blocks,
            input_gate_weight_blocks,
            rate,
            extra,
        ),
        (),
        [(rows, width)],
        [
            normed,
            pltpu.VMEM((rows + 8, width), F32),
            pltpu.VMEM((count, rows, size), F32),
            pltpu.VMEM((count, rows, size), F32),
        ],
        2 * rows * width * features * 8,
    )
    mix_terms = call(
        mixing_kernel,
        (state, *mix_blocks),
        (),
        terms,
        [],
        2 * rows * width * features * 8,
    )
    mixed = (tokens.astype(F32) + share_sums(*mix_terms)).astype(BF16)
    mid = chips_in_order(mixed)
    hidden_width = feedforward_gate_weight.shape[1]
    down_terms = call(
        ffn_kernel,
        (
            mid,
            to_partner(mid),
            feedforward_norm_gain.reshape(4, 2, 1, -1),
            feedforward_gate_scale.reshape(-1, 1, size),
            feedforward_up_scale.reshape(-1, 1, size),
        ),
        (ffn_blocks,),
        terms,
        [
            normed,
            pltpu.VMEM((2, 8 * features, hidden_width), BF16),
            pltpu.VMEM((2, 8 * features, hidden_width // 2), BF16),
            pltpu.SemaphoreType.DMA((4 * PIECES,)),
        ],
        6 * rows * hidden_width * features * 8,
    )
    return (mixed.astype(F32) + share_sums(*down_terms)).astype(BF16)


def solution(mesh):
    torus = Mesh(
        mesh.devices.reshape(mesh.shape["rep"], 4, 8, 4, 2), ("rep", "z", "y", "x", "c")
    )
    return jax.shard_map(
        layer,
        mesh=torus,
        in_specs=(
            P(REP_FS, TP),
            P(),
            P(FS, TP),
            P(TP),
            P(None, TP),
            P(TP, None, None),
            P(TP, None, None),
            P(TP),
            P(REP_FS),
            P(TP, FS),
            P(FS),
            P(),
            P(FS, TP),
            P(TP),
            P(FS, TP),
            P(TP),
            P(TP, FS),
            P(FS),
        ),
        out_specs=P(REP_FS, TP),
        check_vma=False,
    )
```
